32 devices in a mesh: sp: 16 (over z, y, x), tp: 2 (over core).
Axes of the slice: x: 2, y: 2, z: 4, core: 2. Of those that a mesh axis runs over, the one named last changes fastest.
Arguments:
- normed: bfloat16 [4096, 2048], P(('sp', 'tp')), may hold values from -40 to 40
- query_weight: bfloat16 [2048, 2048], P(None, 'tp'), may hold values from -1.5 to 1.5
- key_weight: bfloat16 [2048, 2048], P(None, 'tp'), may hold values from -1 to 1
- value_weight: bfloat16 [2048, 2048], P(None, 'tp'), may hold values from -0.125 to 0.125
- pool_in_weight: bfloat16 [2048, 1024], P(None, 'tp'), may hold values from -0.125 to 0.125
- pool_weight: bfloat16 [8, 128, 128], P('tp'), may hold values from -0.5 to 0.5
- map_balance: float32 [8], replicated, may hold values from 0.3 to 0.8
- head_gain: float32 [256], replicated, may hold values from 0.1 to 1.9
- contrast_out_weight: bfloat16 [2048, 2048], P('tp'), may hold values from -0.109375 to 0.109375
- pool_out_weight: bfloat16 [1024, 2048], P('tp'), may hold values from -0.109375 to 0.109375
Outputs:
- layer_out: bfloat16 [4096, 2048], P(('sp', 'tp'))
The draws below stay inside these ranges and needn't reach their ends.
All inputs are finite; a program needn't handle non-finite values.
Results may differ from the reference program's by a relative error of at most 0.03.
Values may be sent and summed in bfloat16 or wider, within the bound.
No kernel may reach another device: no remote copies, remote signals or barrier semaphores. Data moves between devices by JAX's collectives and lax.ppermute only.
A program may use at most 128 MiB of HBM per device.

```python
import math
import jax
import jax.numpy as jnp
from jax import lax

D = 2048
HEADS = 8
HEAD_DIM = 128
GROUPS = 8
GROUP_WIDTH = 128
TOKENS = 4096
N_TP = 2


def shared_keys(key):
    gaussian = jnp.clip(jax.random.normal(jax.random.fold_in(key, 11), (D, 2 * HEADS * HEAD_DIM), jnp.float32), -6.0, 6.0)
    return gaussian * (1.3 / math.sqrt(D))


def draw_key_weight(key, part):
    return shared_keys(key).astype(jnp.bfloat16)


def draw_query_weight(key, part):
    independent = jnp.clip(jax.random.normal(jax.random.fold_in(key, 12), (D, 2 * HEADS * HEAD_DIM), jnp.float32), -6.0, 6.0) * (1.3 / math.sqrt(D))
    aligned = independent
    return aligned.astype(jnp.bfloat16)


def draw_normed(key, part):
    gaussian = jax.random.normal(jax.random.fold_in(key, 21), (TOKENS, D), jnp.float32)
    return jnp.clip(gaussian, -6.0, 6.0).astype(jnp.bfloat16)


def level_of(own_key, dims, pieces, smallest, high):
    def one(dim, parts):
        heights = jax.random.uniform(jax.random.fold_in(jax.random.fold_in(own_key, 6), dim), (parts,), jnp.float32, smallest / len(pieces), high / len(pieces))
        return jnp.repeat(jnp.exp(heights), dims[dim] // parts).reshape((-1,) + (1,) * (len(dims) - dim - 1))

    gain = one(*pieces[0])
    for cut in pieces[1:]:
        gain = gain * one(*cut)
    return gain


def noise(own_key, dims, scale, most, shards=(), held_as=jnp.bfloat16):
    array = jax.random.normal(own_key, dims, jnp.float32) * scale
    if len(shards) > 0:
        array = level_of(own_key, dims, shards, -0.22, 0.18) * array
    return jnp.clip(array, min=-most, max=most).astype(held_as)


def setup_inputs(seed: int = 0) -> dict:
    streams_of = jax.random.split(jax.random.key(seed), 11)
    normed = draw_normed(jax.random.fold_in(streams_of[10], 71), 0)
    query_weight = draw_query_weight(jax.random.fold_in(streams_of[10], 71), 0)
    key_weight = draw_key_weight(jax.random.fold_in(streams_of[10], 71), 0)
    value_weight = noise(streams_of[3], (D, 2 * HEADS * HEAD_DIM), D ** -0.5, 0.125, ((1, 2),))
    pool_in_weight = noise(streams_of[4], (D, GROUPS * GROUP_WIDTH), D ** -0.5, 0.125, ((1, 2),))
    pool_weight = noise(streams_of[5], (GROUPS, GROUP_WIDTH, GROUP_WIDTH), GROUP_WIDTH ** -0.5, 0.5, ((0, 2),))
    map_balance = jnp.clip(jax.random.uniform(streams_of[6], (HEADS,), jnp.float32, 0.3, 0.8), 0.3, 0.8)
    head_gain = jnp.clip(1.0 + 0.18 * jax.random.normal(streams_of[7], (2 * HEAD_DIM,), jnp.float32), 0.1, 1.9)
    contrast_out_weight = noise(streams_of[8], (2 * HEADS * HEAD_DIM, D), (2 * HEADS * HEAD_DIM + GROUPS * GROUP_WIDTH) ** -0.5, 0.109375, ((0, 2),))
    pool_out_weight = noise(streams_of[9], (GROUPS * GROUP_WIDTH, D), (2 * HEADS * HEAD_DIM + GROUPS * GROUP_WIDTH) ** -0.5, 0.109375, ((0, 2),))
    return {"normed": normed, "query_weight": query_weight, "key_weight": key_weight, "value_weight": value_weight, "pool_in_weight": pool_in_weight, "pool_weight": pool_weight, "map_balance": map_balance, "head_gain": head_gain, "contrast_out_weight": contrast_out_weight, "pool_out_weight": pool_out_weight}


reach_back = 15
norm_epsilon = 1e-06

def map_output(queries, key_rows, value_rows):
    total_rows = queries.shape[0]
    block_rows = math.gcd(total_rows, 1024)
    score_scale = HEAD_DIM ** (-0.5)
    outputs = []
    for block_index in range(total_rows // block_rows):
        first_row = block_index * block_rows
        last_row = first_row + block_rows
        scores = jnp.dot(queries[first_row:last_row], key_rows[:last_row].T, preferred_element_type=jnp.float32) * score_scale
        query_order = first_row + jnp.arange(block_rows, dtype=jnp.int32)
        key_order = jnp.arange(last_row, dtype=jnp.int32)
        scores = jnp.where(key_order[None, :] <= query_order[:, None], scores, -jnp.inf)
        row_peak = lax.optimization_barrier(jnp.max(scores, axis=1, keepdims=True))
        raised = jnp.exp(scores - row_peak)
        row_total = lax.optimization_barrier(jnp.sum(raised, axis=1, keepdims=True))
        weighted = jnp.dot(raised.astype(jnp.bfloat16), value_rows[:last_row], preferred_element_type=jnp.float32)
        outputs.append((weighted / row_total).astype(jnp.bfloat16))
    return jnp.concatenate(outputs, axis=0)

def reference(normed, query_weight, key_weight, value_weight, pool_in_weight, pool_weight, map_balance, head_gain, contrast_out_weight, pool_out_weight):
    queries = jnp.dot(normed, query_weight, preferred_element_type=jnp.float32).astype(jnp.bfloat16)
    key_rows = jnp.dot(normed, key_weight, preferred_element_type=jnp.float32).astype(jnp.bfloat16)
    value_rows = jnp.dot(normed, value_weight, preferred_element_type=jnp.float32).astype(jnp.bfloat16)
    pool_input = jnp.dot(normed, pool_in_weight, preferred_element_type=jnp.float32).astype(jnp.bfloat16)
    value_width = 2 * HEAD_DIM
    head_outputs = []
    for head in range(HEADS):
        maps = []
        for which in range(2):
            column = (2 * head + which) * HEAD_DIM
            result_map = map_output(queries[:, column:column + HEAD_DIM], key_rows[:, column:column + HEAD_DIM], value_rows[:, head * value_width:(head + 1) * value_width])
            maps.append(lax.optimization_barrier(result_map).astype(jnp.float32))
        contrast = maps[0] - map_balance[head] * maps[1]
        mean_square = lax.optimization_barrier(jnp.mean(contrast * contrast, axis=1, keepdims=True))
        head_outputs.append((contrast * lax.rsqrt(mean_square + norm_epsilon) * head_gain).astype(jnp.bfloat16))
    contrast_out = jnp.concatenate(head_outputs, axis=1)
    total_rows = normed.shape[0]
    pool_width = GROUPS * GROUP_WIDTH
    extended = jnp.concatenate([jnp.zeros((reach_back, pool_width), jnp.float32), pool_input.astype(jnp.float32)], axis=0)
    group_index = jnp.arange(pool_width, dtype=jnp.int32) // GROUP_WIDTH
    widths = jnp.left_shift(jnp.int32(2), group_index % 4)
    window_sum = jnp.zeros((total_rows, pool_width), jnp.float32)
    for offset in range(reach_back + 1):
        window_sum = window_sum + extended[reach_back - offset:reach_back - offset + total_rows] * (offset < widths)[None, :].astype(jnp.float32)
    position = jnp.arange(total_rows, dtype=jnp.int32)
    counts = jnp.minimum(position[:, None] + 1, widths[None, :]).astype(jnp.float32)
    spread = (window_sum / counts - extended[reach_back:]).astype(jnp.bfloat16)
    spread = lax.optimization_barrier(spread).astype(jnp.float32)
    mixed_groups = jnp.einsum('sgc,gce->sge', spread.reshape(total_rows, GROUPS, GROUP_WIDTH), pool_weight.astype(jnp.float32))
    pool_out = mixed_groups.reshape(total_rows, pool_width).astype(jnp.bfloat16)
    diff_rows = 2 * HEADS * HEAD_DIM // N_TP
    pool_rows = GROUPS * GROUP_WIDTH // N_TP
    summed = jnp.zeros((total_rows, D), jnp.float32)
    for part_index in range(N_TP):
        low_diff = part_index * diff_rows
        low_pool = part_index * pool_rows
        partial_value = jnp.dot(contrast_out[:, low_diff:low_diff + diff_rows], contrast_out_weight[low_diff:low_diff + diff_rows], preferred_element_type=jnp.float32)
        partial_value = partial_value + jnp.dot(pool_out[:, low_pool:low_pool + pool_rows], pool_out_weight[low_pool:low_pool + pool_rows], preferred_element_type=jnp.float32)
        summed = summed + lax.optimization_barrier(partial_value.astype(jnp.bfloat16)).astype(jnp.float32)
    return summed.astype(jnp.bfloat16)
```

```python
import functools
import math

import jax
import jax.numpy as jnp
from jax import lax
from jax.experimental import pallas as pl
from jax.experimental.pallas import tpu as pltpu
from jax.sharding import PartitionSpec as P

norm_epsilon = 1e-06
halo = 16
log2e = math.log2(math.e)

VMEM = pltpu.VMEM
SMEM = pltpu.SMEM


def dot(a, b):
    return jnp.dot(a, b, preferred_element_type=jnp.float32)


def dot_t(a, b):
    return lax.dot_general(a, b, (((1,), (1,)), ((), ())), preferred_element_type=jnp.float32)


def cost(flops, nbytes, exps=0):
    return pl.CostEstimate(flops=int(flops), bytes_accessed=int(nbytes), transcendentals=int(exps))


def params(*semantics, mib=48):
    return pltpu.CompilerParams(dimension_semantics=semantics, vmem_limit_bytes=mib << 20)


def project_body(n_w, scalars, mine, other, *rest):
    weights, out, rows, acc = rest[:n_w], rest[n_w], rest[n_w + 1], rest[n_w + 2]
    step = pl.program_id(0)
    half = mine.shape[0]
    first = pl.multiple_of(scalars[1] * half, half)
    second = pl.multiple_of((1 - scalars[1]) * half, half)
    rows[pl.ds(first, half), :] = mine[...]
    rows[pl.ds(second, half), :] = other[...]
    x = rows[...]
    width = weights[0].shape[1]
    for n in range(n_w):
        part = dot(x, weights[n][...])
        cols = slice(n * width, (n + 1) * width)

        @pl.when(step == 0)
        def _():
            acc[:, cols] = part

        @pl.when(step > 0)
        def _():
            acc[:, cols] += part

    @pl.when(step == pl.num_programs(0) - 1)
    def _():
        out[...] = acc[...].astype(out.dtype)


def project(head, which, mine, other, weights, width):
    half, depth = mine.shape
    tiles = 4
    tile = depth // tiles
    n_w = len(weights)
    scalars = jnp.stack([head, which]).astype(jnp.int32)
    grid_spec = pltpu.PrefetchScalarGridSpec(
        num_scalar_prefetch=1,
        grid=(tiles,),
        in_specs=[pl.BlockSpec((half, tile), lambda i, sc: (0, i))] * 2
        + [pl.BlockSpec((tile, width), lambda i, sc: (i, sc[0]))] * n_w,
        out_specs=pl.BlockSpec((2 * half, n_w * width), lambda i, sc: (0, 0)),
        scratch_shapes=[
            pltpu.VMEM((2 * half, tile), jnp.bfloat16),
            pltpu.VMEM((2 * half, n_w * width), jnp.float32),
        ],
    )
    return pl.pallas_call(
        functools.partial(project_body, n_w),
        grid_spec=grid_spec,
        out_shape=jax.ShapeDtypeStruct((2 * half, n_w * width), jnp.bfloat16),
        compiler_params=params("arbitrary", mib=24),
        cost_estimate=cost(4 * half * depth * n_w * width, 2 * depth * n_w * width),
        name="project",
    )(scalars, mine, other, *weights)


def pool_body(groups, scalars, mine, other, rim, w_in, w_mix, w_out, out, rows, mixed):
    half = mine.shape[0]
    count = 2 * half
    which, tp_index, sp_index = scalars[0], scalars[1], scalars[2]
    first = pl.multiple_of(halo + which * half, halo)
    second = pl.multiple_of(halo + (1 - which) * half, halo)
    rows[0:halo, :] = rim[...]
    rows[pl.ds(first, half), :] = mine[...]
    rows[pl.ds(second, half), :] = other[...]
    pooled = dot(rows[...], w_in[...]).astype(jnp.bfloat16).astype(jnp.float32)
    index = lax.broadcasted_iota(jnp.int32, pooled.shape, 0)
    pooled = jnp.where((index < halo) & (sp_index == 0), 0.0, pooled)
    sums = []
    total = pooled
    for bit in range(4):
        total = total + pltpu.roll(total, 1 << bit, 0)
        sums.append(total)
    width = w_mix.shape[1]
    position = sp_index * count + lax.broadcasted_iota(jnp.int32, (count, width), 0)
    for g in range(groups):
        kind = lax.rem(tp_index * groups + g, 4)
        cols = slice(g * width, (g + 1) * width)
        picked = sums[0][halo:, cols]
        for bit in range(1, 4):
            picked = jnp.where(kind == bit, sums[bit][halo:, cols], picked)
        window = jnp.left_shift(jnp.int32(2), kind)
        counts = jnp.minimum(position + 1, window).astype(jnp.float32)
        spread = (picked / counts - pooled[halo:, cols]).astype(jnp.bfloat16)
        mixed[:, cols] = dot(spread, w_mix[g]).astype(jnp.bfloat16)
    out[...] = dot(mixed[...], w_out[...])


def pool(which, tp_index, sp_index, mine, other, rim, w_in, w_mix, w_out):
    half, depth = mine.shape
    cols = w_in.shape[1]
    scalars = jnp.stack([which, tp_index, sp_index]).astype(jnp.int32)
    return pl.pallas_call(
        functools.partial(pool_body, w_mix.shape[0]),
        in_specs=[pl.BlockSpec(memory_space=SMEM)] + [pl.BlockSpec(memory_space=VMEM)] * 6,
        out_specs=pl.BlockSpec(memory_space=VMEM),
        out_shape=jax.ShapeDtypeStruct((2 * half, w_out.shape[1]), jnp.float32),
        scratch_shapes=[
            pltpu.VMEM((2 * half + halo, depth), jnp.bfloat16),
            pltpu.VMEM((2 * half, cols), jnp.bfloat16),
        ],
        compiler_params=params(mib=32),
        cost_estimate=cost(8 * half * depth * cols, 8 * depth * cols),
        name="pool",
    )(scalars, mine, other, rim, w_in, w_mix, w_out)


def softmax_parts(scores, old_peak, scale):
    peak = old_peak
    for s in scores:
        top = jnp.max(s, axis=1, keepdims=True)
        peak = top if peak is None else jnp.maximum(peak, top)
    weights, total = [], None
    for s in scores:
        raised = jnp.exp2((s - peak) * scale)
        part = jnp.sum(raised, axis=1, keepdims=True)
        total = part if total is None else total + part
        weights.append(raised.astype(jnp.bfloat16))
    return peak, total, weights


def own_body(heads, rows, scale, scalars, *refs):
    own, partner = refs[:heads], refs[heads : 2 * heads]
    q_out, stat_out, acc_out, keys, values, sems = refs[2 * heads :]
    slot, parity = scalars[0], scalars[1]
    width = keys.shape[1]
    dim = width // 2
    copies = []
    for k in range(heads):
        place = jnp.bitwise_xor(k, slot)
        q_at = pl.multiple_of(place * rows, rows)
        own_at = pl.multiple_of((2 * place + parity) * rows, rows)
        partner_at = pl.multiple_of((2 * place + 1 - parity) * rows, rows)
        for source, target in (
            (own[k].at[:, 0:width], q_out.at[pl.ds(q_at, rows), :]),
            (own[k].at[:, width : 2 * width], keys.at[pl.ds(own_at, rows), :]),
            (own[k].at[:, 2 * width : 3 * width], values.at[pl.ds(own_at, rows), :]),
            (partner[k].at[:, width : 2 * width], keys.at[pl.ds(partner_at, rows), :]),
            (partner[k].at[:, 2 * width : 3 * width], values.at[pl.ds(partner_at, rows), :]),
        ):
            copies.append(pltpu.make_async_copy(source, target, sems.at[len(copies)]))
    for copy in copies:
        copy.start()
    for copy in copies:
        copy.wait()
    lane = lax.broadcasted_iota(jnp.int32, (rows, 128), 1)
    row = lax.broadcasted_iota(jnp.int32, (rows, 2 * rows), 0)
    col = lax.broadcasted_iota(jnp.int32, (rows, 2 * rows), 1)
    allowed = col <= row + parity * rows
    for i in range(heads):
        q_rows = slice(i * rows, (i + 1) * rows)
        for c in range(2):
            cols = slice(c * dim, (c + 1) * dim)
            q = q_out[q_rows, cols]
            before = 2 * i * rows
            scores = []
            if before:
                scores.append(dot_t(q, keys[0:before, cols]))
            edge = dot_t(q, keys[before : before + 2 * rows, cols])
            scores.append(jnp.where(allowed, edge, -jnp.inf))
            peak, total, weights = softmax_parts(scores, None, scale)
            acc = dot(weights[-1], values[before : before + 2 * rows, :])
            if before:
                acc = acc + dot(weights[0], values[0:before, :])
            acc_out[c, q_rows, :] = acc
            stat_out[c, q_rows, :] = jnp.where(lane < 64, peak, total)


def attend_own(slot, parity, own, partner, scale):
    heads = len(own)
    rows, width = own[0].shape[0], own[0].shape[1] // 3
    count = heads * rows
    scalars = jnp.stack([slot, parity]).astype(jnp.int32)
    pairs = 2 * count * 2 * count
    return pl.pallas_call(
        functools.partial(own_body, heads, rows, scale * log2e),
        in_specs=[pl.BlockSpec(memory_space=SMEM)]
        + [pl.BlockSpec(memory_space=pl.ANY)] * (2 * heads),
        out_specs=[pl.BlockSpec(memory_space=VMEM)] * 3,
        out_shape=[
            jax.ShapeDtypeStruct((count, width), jnp.bfloat16),
            jax.ShapeDtypeStruct((2, count, 128), jnp.float32),
            jax.ShapeDtypeStruct((2, count, width), jnp.float32),
        ],
        scratch_shapes=[
            pltpu.VMEM((2 * count, width), jnp.bfloat16),
            pltpu.VMEM((2 * count, width), jnp.bfloat16),
            pltpu.SemaphoreType.DMA((5 * heads,)),
        ],
        compiler_params=params(mib=40),
        cost_estimate=cost(pairs * width * 2, 4 * count * width * 4, pairs),
        name="attend_own",
    )(scalars, *own, *partner)


def cross_body(blocks, heads, rows, scale, final, scalars, balance, gain, q_in, stat_in, acc_in, *refs):
    pieces, outs = refs[:blocks], refs[blocks:]
    width = q_in.shape[1]
    dim = width // 2
    active, slot, head = scalars[0], scalars[1], scalars[2]
    if final:
        done, stat_out, acc_out = outs[heads], outs[heads + 1], outs[heads + 2]
    else:
        stat_out, acc_out = outs
    lane = lax.broadcasted_iota(jnp.int32, (rows, 128), 1)

    @pl.when(active == 1)
    def _():
        for i in range(heads):
            q_rows = slice(i * rows, (i + 1) * rows)
            for c in range(2):
                cols = slice(c * dim, (c + 1) * dim)
                q = q_in[q_rows, cols]
                old_peak = stat_in[c, q_rows, 0:1]
                old_total = stat_in[c, q_rows, 64:65]
                scores = [dot_t(q, piece[:, cols]) for piece in pieces]
                peak, total, weights = softmax_parts(scores, old_peak, scale)
                shrink = jnp.exp2((old_peak - peak) * scale)
                acc = acc_in[c, q_rows, :] * shrink
                for weight, piece in zip(weights, pieces):
                    acc = acc + dot(weight, piece[:, width : 2 * width])
                acc_out[c, q_rows, :] = acc
                stat_out[c, q_rows, :] = jnp.where(lane < 64, peak, old_total * shrink + total)

    @pl.when(active == 0)
    def _():
        stat_out[...] = stat_in[...]
        acc_out[...] = acc_in[...]

    if final:
        factor = balance[head]
        for i in range(heads):
            q_rows = slice(i * rows, (i + 1) * rows)
            maps = [
                (acc_out[c, q_rows, :] / stat_out[c, q_rows, 64:65])
                .astype(jnp.bfloat16)
                .astype(jnp.float32)
                for c in range(2)
            ]
            contrast = maps[0] - factor * maps[1]
            square = jnp.mean(contrast * contrast, axis=1, keepdims=True)
            contrast = contrast * lax.rsqrt(square + norm_epsilon) * gain[...]
            done[q_rows, :] = contrast.astype(jnp.bfloat16)
        for k in range(heads):
            place = jnp.bitwise_xor(k, slot)
            outs[k][...] = done[pl.ds(pl.multiple_of(place * rows, rows), rows), :]


def attend_cross(active, slot, head, balance, gain, state, pieces, heads, scale, final):
    q, stat, acc = state
    count, width = q.shape
    rows = count // heads
    scalars = jnp.stack([active, slot, head]).astype(jnp.int32)
    pairs = 2 * count * rows * len(pieces)
    state_shapes = [
        jax.ShapeDtypeStruct(stat.shape, jnp.float32),
        jax.ShapeDtypeStruct(acc.shape, jnp.float32),
    ]
    if final:
        out_shape = [jax.ShapeDtypeStruct((rows, width), jnp.bfloat16)] * heads
        scratch = [
            pltpu.VMEM((count, width), jnp.bfloat16),
            pltpu.VMEM(stat.shape, jnp.float32),
            pltpu.VMEM(acc.shape, jnp.float32),
        ]
    else:
        out_shape, scratch = state_shapes, []
    return pl.pallas_call(
        functools.partial(cross_body, len(pieces), heads, rows, scale * log2e, final),
        in_specs=[pl.BlockSpec(memory_space=SMEM)] * 2
        + [pl.BlockSpec(memory_space=VMEM)] * (4 + len(pieces)),
        out_specs=[pl.BlockSpec(memory_space=VMEM)] * len(out_shape),
        out_shape=out_shape,
        scratch_shapes=scratch,
        compiler_params=params(mib=48),
        cost_estimate=cost(pairs * width * 3, 8 * count * width, pairs),
        name="attend_cross",
    )(scalars, balance, gain, q, stat, acc, *pieces)


def output_body(heads, scalars, *refs):
    blocks, weight, pooled, out = refs[:heads], refs[heads], refs[heads + 1], refs[heads + 2]
    half, tile = out.shape
    width = blocks[0].shape[1]
    start = pl.multiple_of(scalars[1] * half, half)
    total = pooled[pl.ds(start, half), :]
    for k in range(heads):
        place = jnp.bitwise_xor(k, scalars[0])
        part = weight[pl.ds(pl.multiple_of(place * width, width), width), :]
        total = total + dot(blocks[k][pl.ds(start, half), :], part)
    out[...] = total.astype(out.dtype)


def output(slot, part, blocks, weight, pooled, dtype):
    heads = len(blocks)
    rows, width = blocks[0].shape
    depth, model = weight.shape
    half = rows // 2
    tiles = 4
    tile = model // tiles
    scalars = jnp.stack([slot, part]).astype(jnp.int32)
    grid_spec = pltpu.PrefetchScalarGridSpec(
        num_scalar_prefetch=1,
        grid=(tiles,),
        in_specs=[pl.BlockSpec((rows, width), lambda i, sc: (0, 0))] * heads
        + [
            pl.BlockSpec((depth, tile), lambda i, sc: (0, i)),
            pl.BlockSpec((rows, tile), lambda i, sc: (0, i)),
        ],
        out_specs=pl.BlockSpec((half, tile), lambda i, sc: (0, i)),
    )
    return pl.pallas_call(
        functools.partial(output_body, heads),
        grid_spec=grid_spec,
        out_shape=jax.ShapeDtypeStruct((half, model), dtype),
        compiler_params=params("arbitrary", mib=24),
        cost_estimate=cost(2 * half * depth * model, 2 * depth * model),
        name="output",
    )(scalars, *blocks, weight, pooled)


def per_device(
    normed,
    query_weight,
    key_weight,
    value_weight,
    pool_in_weight,
    pool_weight,
    map_balance,
    head_gain,
    contrast_out_weight,
    pool_out_weight,
):
    sp_count, tp_count = lax.axis_size("sp"), lax.axis_size("tp")
    s, t = lax.axis_index("sp"), lax.axis_index("tp")
    width = head_gain.shape[0]
    dim = width // 2
    heads = query_weight.shape[1] // width
    members = 2 * heads
    groups = sp_count // members
    scale = dim ** (-0.5)
    both = ("sp", "tp")
    swap = [(i, i ^ 1) for i in range(tp_count)]

    def exchange_route(k, first_group, back):
        route = []
        for source in range(first_group * members, sp_count):
            m = source % members
            base = source - m
            for core in range(tp_count):
                local = k ^ (m >> 1)
                target = base + (core & 1) * heads + local
                target_core = (core & ~1) | (m & 1)
                pair = (source * tp_count + core, target * tp_count + target_core)
                route.append(pair[::-1] if back else pair)
        return route

    def spread_out(parts, first_group=0, back=False):
        return [
            lax.ppermute(part, both, exchange_route(k, first_group, back))
            for k, part in enumerate(parts)
        ]

    def across(block):
        return lax.ppermute(block, "tp", swap)

    def whole_rows(block):
        if tp_count == 2:
            return block, across(block), t
        full = lax.all_gather(block, "tp", axis=0, tiled=True)
        half = full.shape[0] // 2
        return full[:half], full[half:], jnp.int32(0)

    member = s % members
    group = s // members
    send_slot = member >> 1
    own_slot = member % heads
    parity = t & 1

    mine, other, which = whole_rows(normed)
    far = [
        lax.ppermute(
            normed, "sp", [(i, i + members) for i in range(sp_count - members)]
        )
    ]
    sent = [
        project(
            jnp.bitwise_xor(k, send_slot),
            which,
            mine,
            other,
            (query_weight, key_weight, value_weight),
            width,
        )
        for k in range(heads)
    ]
    own = spread_out(sent)
    partner = [across(block) for block in own]

    last = jnp.where(which == 0, other[-halo:], mine[-halo:])
    rim = lax.ppermute(last, "sp", [(i, (i + 1) % sp_count) for i in range(sp_count)])
    pooled = pool(
        which, t, s, mine, other, rim, pool_in_weight, pool_weight, pool_out_weight
    )

    q, stat, acc = attend_own(own_slot, parity, own, partner, scale)

    head = (t - parity) * heads + member
    gain = head_gain.reshape(1, width)

    def cross(rows_here, step, stat, acc, first_group, final):
        mine, other, which = whole_rows(rows_here)
        sent = [
            project(
                jnp.bitwise_xor(k, send_slot), which, mine, other, (key_weight, value_weight), width
            )
            for k in range(heads)
        ]
        got = spread_out(sent, first_group)
        pieces = got + [across(block) for block in got]
        active = (group >= step).astype(jnp.int32)
        return attend_cross(
            active, own_slot, head, map_balance, gain, (q, stat, acc), pieces, heads, scale, final
        )

    if groups == 2:
        done = cross(far[0], 1, stat, acc, 1, True)
    else:
        ring = [(i, (i + members) % sp_count) for i in range(sp_count)]

        def body(step, carry):
            rows_here, stat, acc = carry
            stat, acc = cross(rows_here, step, stat, acc, 0, False)
            return lax.ppermute(rows_here, "sp", ring), stat, acc

        rows_here, stat, acc = lax.fori_loop(
            1, groups - 1, body, (lax.ppermute(normed, "sp", ring), stat, acc)
        )
        done = cross(rows_here, groups - 1, stat, acc, 0, True)

    returned = spread_out(done, back=True)
    if tp_count == 2:
        given = output(send_slot, 1 - t, returned, contrast_out_weight, pooled, jnp.bfloat16)
        taken = across(given)
        kept = output(send_slot, t, returned, contrast_out_weight, pooled, jnp.bfloat16)
        return (kept.astype(jnp.float32) + taken.astype(jnp.float32)).astype(jnp.bfloat16)
    halves = [
        output(send_slot, jnp.int32(p), returned, contrast_out_weight, pooled, jnp.bfloat16)
        for p in range(2)
    ]
    return lax.psum_scatter(
        jnp.concatenate(halves, axis=0), "tp", scatter_dimension=0, tiled=True
    )


def solution(mesh):
    return jax.shard_map(
        per_device,
        mesh=mesh,
        in_specs=(
            P(("sp", "tp"), None),
            P(None, "tp"),
            P(None, "tp"),
            P(None, "tp"),
            P(None, "tp"),
            P("tp", None, None),
            P(),
            P(),
            P("tp", None),
            P("tp", None),
        ),
        out_specs=P(("sp", "tp"), None),
        check_vma=False,
    )
```
